32 devices in a mesh: rep: 2 (over x), fs: 8 (over z, y), tp: 2 (over core).
Axes of the slice: x: 2, y: 2, z: 4, core: 2. Of those that a mesh axis runs over, the one named last changes fastest.
Arguments:
- inputs: bfloat16 [2, 3072, 2048], P('rep', 'fs', 'tp'), may hold values from -6 to 6
- gate_proj: bfloat16 [2048, 2816], P('fs', 'tp'), may hold values from -0.125 to 0.125
- value_proj: bfloat16 [2048, 2816], P('fs', 'tp'), may hold values from -0.125 to 0.125
- gate_taps: float32 [3, 2816], replicated, may hold values from -3 to 3
- value_taps: float32 [3, 2816], replicated, may hold values from -3 to 3
- out_grad: bfloat16 [2, 3072, 2816], P('rep', 'fs', 'tp'), may hold values from -6 to 6
Outputs:
- in_grad: bfloat16 [2, 3072, 2048], P('rep', 'fs', 'tp')
- gate_proj_grad: float32 [2048, 2816], P('fs', 'tp')
- value_proj_grad: float32 [2048, 2816], P('fs', 'tp')
- gate_taps_grad: float32 [3, 2816], replicated
- value_taps_grad: float32 [3, 2816], replicated
The draws below stay inside these ranges and needn't reach their ends.
All inputs are finite; a program needn't handle non-finite values.
Results may differ from the reference program's by a relative error of at most 0.013.
Values may be sent and summed in bfloat16 or wider, within the bound.
A program may use at most 128 MiB of HBM per device.

```python
import jax
import jax.numpy as jnp
from jax import lax

D = 2048
FF = 2816
CONV = 3
HID_DEV = 1408
BATCH = 2
SEQ = 3072
ALL_TOKENS = 6144


def raised(drawn, rng, source, target, shards_of, factor):
    owner, partner = [(jnp.arange(drawn.shape[axis_at]) // (drawn.shape[axis_at] // shards_of)).reshape([-1 if axis == axis_at else 1 for axis in range(drawn.ndim)]) for axis_at in (source, target)]
    chosen = jax.random.permutation(rng, shards_of)[partner]
    strong = (owner == chosen) | (owner == (partner + shards_of // 2) % shards_of)
    return jnp.where(strong, factor * drawn, drawn)


def block_scale(stream_key, extent, shards, least, largest):
    def one(position, blocks):
        draws = jax.random.uniform(jax.random.fold_in(jax.random.fold_in(stream_key, 6), position), (blocks,), jnp.float32, least / len(shards), largest / len(shards))
        return jnp.repeat(jnp.exp(draws), extent[position] // blocks).reshape((-1,) + (1,) * (len(extent) - position - 1))

    factor_of = one(*shards[0])
    for cut in shards[1:]:
        factor_of = factor_of * one(*cut)
    return factor_of


def centred(stream_key, extent, deviation, limit, split=(), kind=jnp.bfloat16):
    level = block_scale(stream_key, extent, split, -0.22, 0.18) if split else 1.0
    result = jax.random.normal(stream_key, extent, jnp.float32) * deviation * level
    return jnp.minimum(jnp.maximum(result, -limit), limit).astype(kind)


def bell_draw_with(key, dims, deviation, bound, split, heavy, kind=jnp.bfloat16):
    array = deviation * jax.random.normal(key, dims, jnp.float32)
    if split:
        array = array * block_scale(key, dims, split, -0.22, 0.18)
    return jnp.clip(raised(array, jax.random.fold_in(key, 3), *heavy), -bound, bound).astype(kind)


def setup_inputs(seed: int = 0) -> dict:
    arg_keys = jax.random.split(jax.random.key(seed), 7)
    inputs = bell_draw_with(arg_keys[0], (BATCH, SEQ, D), 1.0, 6.0, ((0, 2), (1, 8), (2, 2)), (1, 2, 8, 2.0))
    gate_proj = centred(arg_keys[1], (D, FF), D ** -0.5, 0.125, ((0, 8), (1, 2)))
    value_proj = centred(arg_keys[2], (D, FF), D ** -0.5, 0.125, ((0, 8), (1, 2)))
    gate_taps = centred(arg_keys[3], (CONV, FF), 0.577, 3.0, (), jnp.float32)
    value_taps = centred(arg_keys[4], (CONV, FF), 0.577, 3.0, (), jnp.float32)
    out_grad = bell_draw_with(arg_keys[5], (BATCH, SEQ, FF), 1.0, 6.0, ((0, 2), (1, 8), (2, 2)), (1, 2, 8, 2.0))
    return dict(inputs=inputs, gate_proj=gate_proj, value_proj=value_proj, gate_taps=gate_taps, value_taps=value_taps, out_grad=out_grad)


def conv_fwd(pre_acts, taps):
    seq_len = pre_acts.shape[0]
    padded = jnp.pad(pre_acts, ((1, 1), (0, 0)))
    return taps[0] * padded[0:seq_len] + taps[1] * padded[1:seq_len + 1] + taps[2] * padded[2:seq_len + 2]


def conv_back(cot_rows, taps):
    seq_len = cot_rows.shape[0]
    padded = jnp.pad(cot_rows, ((1, 1), (0, 0)))
    return taps[0] * padded[2:seq_len + 2] + taps[1] * padded[1:seq_len + 1] + taps[2] * padded[0:seq_len]


def cotangents(gate_mix, value_mix, cot_in):
    sigmoid_gate = jax.nn.sigmoid(gate_mix)
    gate_cot = cot_in * value_mix * (sigmoid_gate * (1.0 + gate_mix * (1.0 - sigmoid_gate)))
    value_cot = cot_in * (gate_mix * sigmoid_gate)
    return gate_cot, value_cot


def reference(inputs, gate_proj, value_proj, gate_taps, value_taps, out_grad):
    contract_cols = (((1,), (1,)), ((), ()))
    contract_rows = (((0,), (0,)), ((), ()))

    def one_sequence(pair):
        seq_inputs, seq_cot = pair
        seq_len = seq_inputs.shape[0]
        gate_pre = jnp.dot(seq_inputs, gate_proj, preferred_element_type=jnp.float32).astype(jnp.bfloat16)
        value_pre = jnp.dot(seq_inputs, value_proj, preferred_element_type=jnp.float32).astype(jnp.bfloat16)
        gate_mix = conv_fwd(gate_pre.astype(jnp.float32), gate_taps)
        value_mix = conv_fwd(value_pre.astype(jnp.float32), value_taps)
        gate_cot, value_cot = cotangents(gate_mix, value_mix, seq_cot.astype(jnp.float32))
        gate_pre_cot = conv_back(gate_cot, gate_taps).astype(jnp.bfloat16)
        value_pre_cot = conv_back(value_cot, value_taps).astype(jnp.bfloat16)

        def add_block(total, block_index):
            first_col = (block_index * HID_DEV).astype(jnp.int32)
            gate_cols = lax.dynamic_slice_in_dim(gate_pre_cot, first_col, HID_DEV, 1)
            value_cols = lax.dynamic_slice_in_dim(value_pre_cot, first_col, HID_DEV, 1)
            gate_block = lax.dynamic_slice_in_dim(gate_proj, first_col, HID_DEV, 1)
            value_block = lax.dynamic_slice_in_dim(value_proj, first_col, HID_DEV, 1)
            partial_value = lax.dot_general(gate_cols, gate_block, contract_cols, preferred_element_type=jnp.float32)
            partial_value = partial_value + lax.dot_general(value_cols, value_block, contract_cols, preferred_element_type=jnp.float32)
            rounded = lax.optimization_barrier(partial_value.astype(jnp.bfloat16))
            return total + rounded.astype(jnp.float32), None

        in_sum, _ = lax.scan(add_block, jnp.zeros((seq_len, D), jnp.float32), jnp.arange(FF // HID_DEV).astype(jnp.int32))
        in_grad = in_sum.astype(jnp.bfloat16)
        gate_grad = lax.dot_general(seq_inputs, gate_pre_cot, contract_rows, preferred_element_type=jnp.float32)
        value_grad = lax.dot_general(seq_inputs, value_pre_cot, contract_rows, preferred_element_type=jnp.float32)
        gate_padded = jnp.pad(gate_pre.astype(jnp.float32), ((1, 1), (0, 0)))
        value_padded = jnp.pad(value_pre.astype(jnp.float32), ((1, 1), (0, 0)))
        gate_tgrad = jnp.stack([jnp.sum(gate_padded[offset:offset + seq_len] * gate_cot, axis=0) for offset in range(3)])
        value_tgrad = jnp.stack([jnp.sum(value_padded[offset:offset + seq_len] * value_cot, axis=0) for offset in range(3)])
        return in_grad, gate_grad, value_grad, gate_tgrad, value_tgrad

    results = lax.map(one_sequence, (inputs, out_grad))
    factor = float(ALL_TOKENS) ** -0.5
    return (results[0], jnp.sum(results[1], axis=0) * factor, jnp.sum(results[2], axis=0) * factor,
            jnp.sum(results[3], axis=0) * factor, jnp.sum(results[4], axis=0) * factor)
```

```python
import jax
import jax.numpy as jnp
from jax import lax
from jax.sharding import PartitionSpec as P

HALO = 8


def shift(x, axis, step):
    count = lax.axis_size(axis)
    return lax.ppermute(x, axis, [(i, (i + step) % count) for i in range(count)])


def with_halo(rows):
    count = lax.axis_size("fs")
    nxt = lax.ppermute(rows[:HALO], "fs", [(i + 1, i) for i in range(count - 1)])
    prv = lax.ppermute(rows[rows.shape[0] - HALO:], "fs", [(i, i + 1) for i in range(count - 1)])
    return jnp.concatenate([rows, nxt, prv], axis=0)


def before(x):
    return jnp.concatenate([x[:, -1:], x[:, :-1]], axis=1)


def after(x):
    return jnp.concatenate([x[:, 1:], x[:, :1]], axis=1)


def shards(inputs, gate_proj, value_proj, gate_taps, value_taps, out_grad):
    contract_cols = (((1,), (1,)), ((), ()))
    contract_rows = (((0,), (0,)), ((), ()))
    reps, fs_count = lax.axis_size("rep"), lax.axis_size("fs")
    rep = lax.axis_index("rep")
    tokens, feats = inputs.shape[1:]
    hid = gate_proj.shape[1]
    width = min(hid, -(-hid // reps // 128) * 128)
    last = hid - width

    def start_of(part):
        return jnp.minimum(part * width, last)

    first = start_of(rep)
    dead = rep * width - first
    live = jnp.arange(width) >= dead

    def part_cols(x, part):
        return lax.dynamic_slice_in_dim(x, start_of(part), width, x.ndim - 1)

    w_own = jnp.concatenate(
        [jnp.where(live, part_cols(w, rep), jnp.zeros((), w.dtype)) for w in (gate_proj, value_proj)], axis=1
    )
    w_all = lax.all_gather(w_own, "fs", axis=0, tiled=True)

    x_ext = with_halo(inputs[0])
    g_ext = with_halo(out_grad[0])
    x_blocks, g_blocks = [x_ext], [part_cols(g_ext, rep)]
    for step in range(1, reps):
        x_blocks.append(shift(x_ext, "rep", step))
        g_blocks.append(shift(part_cols(g_ext, (rep + step) % reps), "rep", step))
    x_all = lax.all_gather(jnp.stack(x_blocks), "tp", axis=2, tiled=True)
    g_all = jnp.stack(g_blocks).astype(jnp.float32)

    ext = tokens + 2 * HALO
    pre = jnp.dot(x_all.reshape(reps * ext, -1), w_all, preferred_element_type=jnp.float32)
    pre = pre.astype(jnp.bfloat16).astype(jnp.float32).reshape(reps, ext, 2 * width)
    tap_start = lax.axis_index("tp") * hid + first
    taps = jnp.concatenate(
        [lax.dynamic_slice_in_dim(t, tap_start, width, 1) for t in (gate_taps, value_taps)], axis=1
    )
    pre_b, pre_a = before(pre), after(pre)
    mix = taps[0] * pre_b + taps[1] * pre + taps[2] * pre_a
    gate_mix, value_mix = mix[..., :width], mix[..., width:]
    sig = jax.nn.sigmoid(gate_mix)
    gate_cot = g_all * value_mix * (sig * (1.0 + gate_mix * (1.0 - sig)))
    value_cot = g_all * (gate_mix * sig)
    cot = jnp.concatenate([gate_cot, value_cot], axis=2)
    pre_cot = taps[0] * after(cot) + taps[1] * cot + taps[2] * before(cot)
    pre_cot = pre_cot[:, :tokens].astype(jnp.bfloat16).reshape(reps * tokens, 2 * width)
    tap_terms = jnp.stack(
        [jnp.sum(p[:, :tokens] * cot[:, :tokens], axis=(0, 1)) for p in (pre_b, pre, pre_a)]
    )
    factor = float(tokens * fs_count * reps) ** (-0.5)

    grads = lax.dot_general(
        x_all[:, :tokens].reshape(reps * tokens, -1), pre_cot, contract_rows, preferred_element_type=jnp.float32
    )
    grads = (grads * factor).astype(jnp.bfloat16)
    own = lax.psum_scatter(grads, "fs", scatter_dimension=0, tiled=True)

    partial_value = lax.dot_general(pre_cot, w_all, contract_cols, preferred_element_type=jnp.float32)
    partial_value = lax.psum_scatter(
        partial_value.astype(jnp.bfloat16), "tp", scatter_dimension=1, tiled=True
    ).reshape(reps, tokens, feats)
    in_grad = partial_value[0].astype(jnp.float32)
    for step in range(1, reps):
        in_grad += shift(partial_value[step], "rep", -step).astype(jnp.float32)

    blocks = [own]
    for step in range(1, reps):
        blocks.append(shift(own, "rep", step))
    proj_grads = []
    for branch in range(2):
        cols = jnp.zeros((own.shape[0], hid), jnp.bfloat16)
        cut = [b[:, branch * width : (branch + 1) * width] for b in blocks]
        for step in range(reps):
            part = (rep - step) % reps
            place = start_of(part)
            skip = part * width - place
            old = lax.dynamic_slice_in_dim(cols, place, width, 1)
            new = jnp.where(jnp.arange(width) >= skip, cut[step], old)
            cols = lax.dynamic_update_slice_in_dim(cols, new, place, 1)
        proj_grads.append(cols.astype(jnp.float32))

    tap_sum = lax.psum(tap_terms * factor, "fs").reshape(3, 2, width)
    tap_all = lax.all_gather(lax.all_gather(tap_sum, "rep"), "tp")
    halves = []
    for half in range(tap_all.shape[0]):
        cols = [tap_all[half, p, :, :, max(0, p * width - last) if p * width > last else 0 :] for p in range(reps)]
        halves.append(jnp.concatenate(cols, axis=2))
    taps_out = jnp.concatenate(halves, axis=2)
    return in_grad.astype(jnp.bfloat16)[None], proj_grads[0], proj_grads[1], taps_out[:, 0], taps_out[:, 1]


def solution(mesh):
    placed = (P("rep", "fs", "tp"), P("fs", "tp"), P("fs", "tp"), P(), P(), P("rep", "fs", "tp"))
    return jax.shard_map(
        shards,
        mesh=mesh,
        in_specs=placed,
        out_specs=(P("rep", "fs", "tp"), P("fs", "tp"), P("fs", "tp"), P(), P()),
        check_vma=False,
    )
```
